32 devices in a mesh: grp: 2 (over y), sp: 4 (over z), tp: 4 (over x, core).
Axes of the slice: x: 2, y: 2, z: 4, core: 2. Of those that a mesh axis runs over, the one named last changes fastest.
Arguments:
- queries: bfloat16 [4096, 2048], P(('grp', 'sp'), 'tp'), parts along dimension 0, may hold values from -6 to 6
- key_vectors: bfloat16 [4096, 2048], P(('grp', 'sp'), 'tp'), parts along dimension 0, may hold values from -6 to 6
- value_vectors: bfloat16 [4096, 2048], P(('grp', 'sp'), 'tp'), parts along dimension 0, may hold values from -6 to 6
- forget_sums: float32 [4096, 16], P(('grp', 'sp'), 'tp'), parts along dimension 0, may hold values from -2048 to 0, as said below
- residual: bfloat16 [4096, 2048], P(('grp', 'sp'), 'tp'), parts along dimension 0, may hold values from -20 to 20
- query_gain: float32 [128], replicated, may hold values from 0.5 to 5
- key_gain: float32 [128], replicated, may hold values from 0.5 to 5
- out_weight: bfloat16 [2048, 2048], P(None, 'tp'), may hold values from -0.125 to 0.125
- norm_gain: float32 [2048], replicated, may hold values from 0.1 to 1.9
- gate_weight: bfloat16 [2048, 5504], P('sp', 'tp'), may hold values from -0.125 to 0.125
- up_weight: bfloat16 [2048, 5504], P('sp', 'tp'), may hold values from -0.125 to 0.125
- down_weight: bfloat16 [2048, 5504], P('sp', 'tp'), may hold values from -0.078125 to 0.078125
Outputs:
- layer_output: bfloat16 [4096, 2048], P(('grp', 'sp'), 'tp'), parts along dimension 0
The draws below stay inside these ranges and needn't reach their ends.
There are 2 independent parts, one for each index of `grp`. The reference program is written for one: setup_inputs(seed, part) draws one part's arguments, and reference() takes and returns one part's arrays. A program takes and returns all parts, laid end to end along the dimension named above; an argument that names none is the same for every part. Nothing has to cross between parts.
Inputs may be any that keep to these rules, and one draw needn't show every extreme that they name: `forget_sums`: along positions each head's values never rise.
All inputs are finite; a program needn't handle non-finite values.
Results may differ from the reference program's by a relative error of at most 0.011.
Values may be sent and summed in bfloat16 or wider, within the bound.
A program may use at most 128 MiB of HBM per device.

```python
import math
import jax
import jax.numpy as jnp
from jax import lax

D = 2048
HEADS = 16
HEAD = 128
FF = 5504
TOK_DEV = 512
TOKENS = 2048
N_TP = 4


def paired_rows(key):
    base = jax.random.fold_in(key, 101)
    first, second = jax.random.split(base, 2)
    width = HEADS * HEAD
    query_rows = jax.random.normal(first, (TOKENS, width), jnp.float32)
    key_rows = jax.random.normal(second, (TOKENS, width), jnp.float32)
    return (jnp.clip(query_rows, -6.0, 6.0), jnp.clip(key_rows, -6.0, 6.0))


def draw_queries(key, part):
    return paired_rows(key)[0].astype(jnp.bfloat16)


def draw_key_vectors(key, part):
    return paired_rows(key)[1].astype(jnp.bfloat16)


def draw_gain_common(key, salt):
    inner = jax.random.fold_in(key, salt)
    return jnp.exp(jax.random.uniform(inner, (HEAD,), jnp.float32, math.log(0.5), math.log(2.0)))


def draw_query_gain(key, part):
    return draw_gain_common(key, 201)


def draw_key_gain(key, part):
    return draw_gain_common(key, 202)


def draw_forget_sums(key, part):
    base = jax.random.fold_in(key, 301)
    parts = jax.random.split(base, 7)
    order = jax.random.permutation(parts[0], HEADS)
    fast = order < HEADS // 2
    fast_rate = jnp.exp(jax.random.uniform(parts[1], (HEADS,), jnp.float32, math.log(1.0 / 80.0), math.log(1.0 / 30.0)))
    slow_rate = jnp.exp(jax.random.uniform(parts[2], (HEADS,), jnp.float32, math.log(0.5), math.log(2.0))) * (0.4 / TOKENS)
    rate = jnp.where(fast, fast_rate, slow_rate)
    noise = jnp.exp(jax.random.uniform(parts[3], (TOKENS, HEADS), jnp.float32, math.log(0.5), math.log(2.0)))
    block_factor = jnp.exp(jax.random.uniform(parts[4], (TOKENS // TOK_DEV,), jnp.float32, math.log(0.5), math.log(2.0)))
    block_factor = jnp.repeat(block_factor, TOK_DEV)
    log_gates = -rate[None, :] * noise * block_factor[:, None]
    places = jax.random.randint(parts[5], (3,), 0, TOKENS)
    drops = jnp.log(jax.random.uniform(parts[6], (3, HEADS), jnp.float32, 0.5, 0.8))
    marks = (jnp.arange(TOKENS)[:, None] == places[None, :]).astype(jnp.float32)
    log_gates = log_gates + jnp.dot(marks, drops)
    return jnp.cumsum(log_gates, axis=0)


def draw_residual(key, part):
    base = jax.random.fold_in(key, 401)
    parts = jax.random.split(base, 3)
    column_scale = jnp.exp(jnp.linspace(math.log(0.4), math.log(3.0), D)) * jnp.exp(jax.random.uniform(parts[0], (D,), jnp.float32, math.log(0.7), math.log(1.4)))
    rows = jnp.clip(jax.random.normal(parts[2], (TOKENS, D), jnp.float32), -5.0, 5.0)
    return jnp.clip(rows * column_scale[None, :], -20.0, 20.0).astype(jnp.bfloat16)


def level_of(stream_key, dims, pieces, smallest, top_value):
    def one(axis_at, shards_of):
        draws = jax.random.uniform(jax.random.fold_in(jax.random.fold_in(stream_key, 6), axis_at), (shards_of,), jnp.float32, smallest / len(pieces), top_value / len(pieces))
        return jnp.repeat(jnp.exp(draws), dims[axis_at] // shards_of).reshape((-1,) + (1,) * (len(dims) - axis_at - 1))

    level = one(*pieces[0])
    for cut in pieces[1:]:
        level = level * one(*cut)
    return level


def scatter_about(rng, extent, deviation, limit, shards=(), kind=jnp.bfloat16):
    level = level_of(rng, extent, shards, -0.22, 0.18) if shards else 1.0
    drawn = jax.random.normal(rng, extent, jnp.float32) * deviation * level
    return jnp.minimum(jnp.maximum(drawn, -limit), limit).astype(kind)


def setup_inputs(seed: int = 0, part: int = 0) -> dict:
    key_of = jax.random.split(jax.random.key(seed), 13)
    own_keys = jax.random.split(jax.random.fold_in(key_of[12], part), 13)
    queries = draw_queries(jax.random.fold_in(jax.random.fold_in(key_of[12], part), 71), part)
    key_vectors = draw_key_vectors(jax.random.fold_in(jax.random.fold_in(key_of[12], part), 71), part)
    value_vectors = scatter_about(own_keys[2], (TOKENS, HEADS * HEAD), 1.0, 6.0, ((0, 4), (1, 4)))
    forget_sums = draw_forget_sums(jax.random.fold_in(jax.random.fold_in(key_of[12], part), 71), part)
    residual = draw_residual(jax.random.fold_in(jax.random.fold_in(key_of[12], part), 71), part)
    query_gain = draw_query_gain(jax.random.fold_in(key_of[12], 71), part)
    key_gain = draw_key_gain(jax.random.fold_in(key_of[12], 71), part)
    out_weight = scatter_about(key_of[7], (HEADS * HEAD, D), (HEADS * HEAD) ** -0.5, 0.125, ((1, 4),))
    norm_gain = jnp.clip(1.0 + 0.18 * jax.random.normal(key_of[8], (D,), jnp.float32), 0.1, 1.9)
    gate_weight = scatter_about(key_of[9], (D, FF), D ** -0.5, 0.125, ((0, 4), (1, 4)))
    up_weight = scatter_about(key_of[10], (D, FF), D ** -0.5, 0.125, ((0, 4), (1, 4)))
    down_weight = scatter_about(key_of[11], (D, FF), FF ** -0.5, 0.078125, ((0, 4), (1, 4)))
    return {"queries": queries, "key_vectors": key_vectors, "value_vectors": value_vectors, "forget_sums": forget_sums, "residual": residual, "query_gain": query_gain, "key_gain": key_gain, "out_weight": out_weight, "norm_gain": norm_gain, "gate_weight": gate_weight, "up_weight": up_weight, "down_weight": down_weight}


eps = 1e-06

def head_norm(rows_in, gain):
    count = rows_in.shape[0]
    split = rows_in.reshape(count, -1, HEAD).astype(jnp.float32)
    factor = lax.rsqrt(lax.optimization_barrier(jnp.mean(split * split, axis=2, keepdims=True)) + eps)
    return (split * factor * gain).astype(jnp.bfloat16)

def reference(queries, key_vectors, value_vectors, forget_sums, residual, query_gain, key_gain, out_weight, norm_gain, gate_weight, up_weight, down_weight):
    query_norm = head_norm(queries, query_gain)
    key_norm = lax.optimization_barrier(head_norm(key_vectors, key_gain)).astype(jnp.float32)
    values = value_vectors.reshape(TOKENS, HEADS, HEAD).astype(jnp.float32)
    biases = forget_sums.T
    block = math.gcd(TOKENS, 512)
    key_pos = jnp.arange(TOKENS, dtype=jnp.int32)
    factor = 1.0 / math.sqrt(HEAD)

    def attend(index):
        first = index * block
        query_block = lax.optimization_barrier(lax.dynamic_slice_in_dim(query_norm, first, block, 0)).astype(jnp.float32)
        scores = jnp.einsum('qhd,khd->hqk', query_block, key_norm) * factor
        query_bias = lax.dynamic_slice_in_dim(biases, first, block, 1)
        scores = scores + query_bias[:, :, None] - biases[:, None, :]
        query_pos = first + jnp.arange(block, dtype=jnp.int32)
        allowed = key_pos[None, :] <= query_pos[:, None]
        scores = jnp.where(allowed[None], scores, -jnp.inf)
        top = lax.optimization_barrier(jnp.max(scores, axis=2, keepdims=True))
        raised = jnp.exp(scores - top)
        totals = lax.optimization_barrier(jnp.sum(raised, axis=2))
        weights = lax.optimization_barrier(raised.astype(jnp.bfloat16)).astype(jnp.float32)
        summed = jnp.einsum('hqk,khd->qhd', weights, values)
        return (summed / totals.T[:, :, None]).astype(jnp.bfloat16)
    attended = lax.map(attend, jnp.arange(TOKENS // block, dtype=jnp.int32)).reshape(TOKENS, HEADS * HEAD)
    projected = jnp.dot(attended, out_weight, preferred_element_type=jnp.float32)
    middle = (residual.astype(jnp.float32) + projected).astype(jnp.bfloat16)
    whole = middle.astype(jnp.float32)
    normed = (whole * lax.rsqrt(lax.optimization_barrier(jnp.mean(whole * whole, axis=1, keepdims=True)) + eps) * norm_gain).astype(jnp.bfloat16)
    gate = jnp.dot(normed, gate_weight, preferred_element_type=jnp.float32)
    upward = jnp.dot(normed, up_weight, preferred_element_type=jnp.float32)
    hidden = (jax.nn.silu(gate) * upward).astype(jnp.bfloat16)
    width = FF // N_TP

    def add_block(index, total):
        start = (index * width).astype(jnp.int32)
        hidden_part = lax.dynamic_slice_in_dim(hidden, start, width, 1)
        weight_part = lax.dynamic_slice_in_dim(down_weight, start, width, 1)
        partial_value = lax.dot_general(hidden_part, weight_part, (((1,), (1,)), ((), ())), preferred_element_type=jnp.float32)
        rounded = lax.optimization_barrier(partial_value.astype(jnp.bfloat16))
        return total + rounded.astype(jnp.float32)
    down = lax.fori_loop(0, N_TP, add_block, jnp.zeros((TOKENS, D), jnp.float32))
    return (whole + down).astype(jnp.bfloat16)
```

```python
import math

import jax
import jax.numpy as jnp
from jax import lax
from jax.sharding import PartitionSpec as P


HEAD = 128


eps = 1e-06


def head_norm(rows_in, gain):
    count = rows_in.shape[0]
    split = rows_in.reshape(count, -1, HEAD).astype(jnp.float32)
    factor = lax.rsqrt(jnp.mean(split * split, axis=2, keepdims=True) + eps)
    return (split * factor * gain).astype(jnp.bfloat16)


def relay(block, n):
    arrived = []
    for step in range(n - 1):
        block = lax.ppermute(block, "sp", [(i, i + 1) for i in range(step, n - 1)])
        arrived.append(block)
    return arrived


def tp_shift(block, tp, distance, flip):
    cores = 2 if tp % 2 == 0 else 1
    chips = tp // cores
    perm = []
    for u in range(tp):
        chip, core = u // cores, u % cores
        source = ((chip + distance) % chips) * cores + (core ^ flip)
        perm.append((source, u))
    return lax.ppermute(block, "tp", perm)


def tp_pieces(block, tp):
    cores = 2 if tp % 2 == 0 else 1
    chips = tp // cores
    me = lax.axis_index("tp")
    chip, core = me // cores, lax.rem(me, cores)
    pieces = []
    for d in range(chips):
        piece = block if d == 0 else tp_shift(block, tp, d, 0)
        other_chip = lax.rem(chip + d, chips)
        pieces.append((other_chip * cores + core, piece))
        if cores == 2:
            flipped = tp_shift(piece, tp, 0, 1)
            pieces.append((other_chip * cores + 1 - core, flipped))
    return pieces


def tp_sum_scatter(terms, tp):
    cores = 2 if tp % 2 == 0 else 1
    chips = tp // cores
    rows, width = terms.shape[0], terms.shape[1] // tp
    me = lax.axis_index("tp")
    chip, core = me // cores, lax.rem(me, cores)
    if cores == 2:
        split = terms.reshape(rows, chips, 2, width)
        first = split[:, :, 0].reshape(rows, chips * width)
        second = split[:, :, 1].reshape(rows, chips * width)
        keep = jnp.where(core == 0, first, second)
        give = jnp.where(core == 0, second, first)
        both = keep.astype(jnp.float32) + tp_shift(give, tp, 0, 1).astype(jnp.float32)
    else:
        both = terms.astype(jnp.float32)
    total = lax.dynamic_slice_in_dim(both, chip * width, width, 1)
    rounded = both.astype(jnp.bfloat16)
    for d in range(1, chips):
        target = lax.rem(chip + chips - d, chips)
        sent = lax.dynamic_slice_in_dim(rounded, target * width, width, 1)
        total = total + tp_shift(sent, tp, d, 0).astype(jnp.float32)
    return total


def down_chunks(shape, n, groups):
    rows, columns = shape
    large = n * rows // groups * columns * 2 >= 2 << 20
    return 2 if large and rows % (2 * groups) == 0 else 1


def local(
    n,
    groups,
    tp,
    queries,
    key_vectors,
    value_vectors,
    forget_sums,
    residual,
    query_gain,
    key_gain,
    out_weight,
    norm_gain,
    gate_weight,
    up_weight,
    down_weight,
):
    local_rows = queries.shape[0]
    me = lax.axis_index("sp")
    grp = lax.axis_index("grp")
    heads_here = queries.shape[1] // HEAD
    key_norm = head_norm(key_vectors, key_gain).reshape(local_rows, heads_here * HEAD)
    bias = forget_sums.T
    key_blocks = [key_norm] + relay(key_norm, n)
    value_blocks = [value_vectors] + relay(value_vectors, n)
    bias_blocks = [bias] + relay(bias, n)

    def gathered(weight, name, chunk=0, chunks=1):
        share = weight.shape[0] // groups
        size = share // chunks

        def own(t):
            start = lax.rem(grp + t, groups) * share + chunk * size
            return lax.dynamic_slice_in_dim(weight, start, size, 0)

        mine = lax.all_gather(own(0), "sp", axis=0, tiled=True)
        others = [own(t) for t in range(1, groups)]
        return name, mine, others, size

    def swapped(held, after=None):
        _, mine, others, size = held
        if after is not None:
            mine, _ = lax.optimization_barrier((mine, after))
        pieces = [mine]
        for t in range(1, groups):
            perm = [((a + t) % groups, a) for a in range(groups)]
            other = lax.dynamic_update_slice_in_dim(
                jnp.zeros_like(mine), others[t - 1], me * size, 0
            )
            for s in range(1, n):
                start = lax.rem(me + s, n) * size
                sent = lax.dynamic_slice_in_dim(mine, start, size, 0)
                received = lax.ppermute(sent, "grp", perm)
                other = lax.dynamic_update_slice_in_dim(other, received, start, 0)
                after = received
            pieces.append(other)
        return pieces, after

    gate_weight, up_weight, down_weight, _, _ = lax.optimization_barrier(
        (gate_weight, up_weight, down_weight, value_blocks[-1], key_blocks[-1])
    )
    gate_pieces, _ = swapped(gathered(gate_weight, "gate"))
    up_held = gathered(up_weight, "up")
    chunks = down_chunks(down_weight.shape, n, groups)
    down_held = [gathered(down_weight, f"down{c}", c, chunks) for c in range(chunks)]

    query_norm = head_norm(queries, query_gain)
    factor_scale = 1.0 / math.sqrt(HEAD)
    state = (
        jnp.full((heads_here, local_rows), -1e30, jnp.float32),
        jnp.zeros((heads_here, local_rows), jnp.float32),
        jnp.zeros((local_rows, heads_here, HEAD), jnp.float32),
    )
    per_turn = max(1, min(n, 2048 // local_rows))
    row_pos = lax.iota(jnp.int32, local_rows)
    for first in range(0, n, per_turn):
        members = list(range(first, min(n, first + per_turn)))
        key_block = jnp.concatenate([key_blocks[s] for s in members], 0)
        value_block = jnp.concatenate([value_blocks[s] for s in members], 0)
        key_bias = jnp.concatenate([bias_blocks[s] for s in members], 1)
        block = key_block.shape[0]
        key_block = key_block.reshape(block, heads_here, HEAD)
        value_block = value_block.reshape(block, heads_here, HEAD)
        key_pos = jnp.concatenate([(me - s) * local_rows + row_pos for s in members], 0)
        query_pos = me * local_rows + row_pos

        def live(inner):
            running_max, running_sum, weighted = inner
            scores = (
                jnp.einsum(
                    "qhd,khd->hqk", query_norm, key_block, preferred_element_type=jnp.float32
                )
                * factor_scale
            )
            scores = scores + bias[:, :, None] - key_bias[:, None, :]
            allowed = (key_pos[None, :] <= query_pos[:, None]) & (key_pos[None, :] >= 0)
            scores = jnp.where(allowed[None], scores, -1e30)
            new_max = jnp.maximum(running_max, jnp.max(scores, axis=2))
            raised = jnp.where(allowed[None], jnp.exp(scores - new_max[:, :, None]), 0.0)
            shrink = jnp.exp(running_max - new_max)
            running_sum = shrink * running_sum + jnp.sum(raised, axis=2)
            update = jnp.einsum(
                "hqk,khd->qhd",
                raised.astype(jnp.bfloat16),
                value_block,
                preferred_element_type=jnp.float32,
            )
            weighted = weighted * shrink.T[:, :, None] + update
            return (new_max, running_sum, weighted)

        if first == 0:
            state = live(state)
        else:
            state = lax.cond(me >= first, live, lambda inner: inner, state)
    _, running_sum, weighted = state
    attended = (
        (weighted / running_sum.T[:, :, None])
        .astype(jnp.bfloat16)
        .reshape(local_rows, heads_here * HEAD)
    )
    width = heads_here * HEAD
    projected = sum(
        jnp.dot(
            piece,
            lax.dynamic_slice_in_dim(out_weight, index * width, width, 0),
            preferred_element_type=jnp.float32,
        )
        for index, piece in tp_pieces(attended, tp)
    )
    middle = (residual.astype(jnp.float32) + projected).astype(jnp.bfloat16)
    columns = middle.shape[1]
    whole_rows = jnp.zeros((local_rows, columns * tp), jnp.bfloat16)
    stream = tp_pieces(middle, tp)
    after = tuple(piece for _, piece in stream)
    up_pieces, after = swapped(up_held, after)
    down_pieces = []
    for held in down_held:
        pieces, after = swapped(held, after)
        down_pieces.append(pieces)
    for index, piece in stream:
        whole_rows = lax.dynamic_update_slice_in_dim(whole_rows, piece, index * columns, 1)
    whole_rows = whole_rows.astype(jnp.float32)
    normed = (
        whole_rows
        * lax.rsqrt(jnp.mean(whole_rows * whole_rows, axis=1, keepdims=True) + eps)
        * norm_gain
    ).astype(jnp.bfloat16)

    share = gate_weight.shape[0] // groups
    split = normed.reshape(local_rows, n, groups, share)
    normed_shares = [split[:, :, k].reshape(local_rows, n * share) for k in range(groups)]

    def rotated(items, t):
        out = items[t % groups]
        for k in range(1, groups):
            out = jnp.where(grp == k, items[(k + t) % groups], out)
        return out

    ordered = [rotated(normed_shares, t) for t in range(groups)]

    def times(pieces):
        return sum(
            jnp.dot(rows, piece, preferred_element_type=jnp.float32)
            for rows, piece in zip(ordered, pieces)
        )

    gate = times(gate_pieces)
    upward = times(up_pieces)
    hidden = (jax.nn.silu(gate) * upward).astype(jnp.bfloat16)
    size = share // chunks
    summed = []
    for c in range(chunks):
        for t in range(groups):
            terms = lax.dot_general(
                hidden, down_pieces[c][t], (((1,), (1,)), ((), ())),
                preferred_element_type=jnp.float32,
            ).astype(jnp.bfloat16)
            summed.append(tp_sum_scatter(terms, tp).reshape(local_rows, n // tp, size))
    in_order = []
    for k in range(groups):
        for c in range(chunks):
            of_chunk = summed[c * groups : (c + 1) * groups]
            item = of_chunk[k]
            for g in range(1, groups):
                item = jnp.where(grp == g, of_chunk[(k - g) % groups], item)
            in_order.append(item)
    summed = jnp.stack(in_order, 2).reshape(local_rows, middle.shape[1])
    return (middle.astype(jnp.float32) + summed).astype(jnp.bfloat16)


def solution(mesh):
    placed = (
        P(("grp", "sp"), "tp"),
        P(("grp", "sp"), "tp"),
        P(("grp", "sp"), "tp"),
        P(("grp", "sp"), "tp"),
        P(("grp", "sp"), "tp"),
        P(),
        P(),
        P(None, "tp"),
        P(),
        P("sp", "tp"),
        P("sp", "tp"),
        P("sp", "tp"),
    )
    n, groups, tp = mesh.shape["sp"], mesh.shape["grp"], mesh.shape["tp"]

    def body(*args):
        return local(n, groups, tp, *args)

    return jax.shard_map(
        body, mesh=mesh, in_specs=placed, out_specs=P(("grp", "sp"), "tp"), check_vma=False
    )
```
